32 devices in a mesh: sp: 8 (over z, x), tp: 4 (over y, core).
Axes of the slice: x: 2, y: 2, z: 4, core: 2. Of those that a mesh axis runs over, the one named last changes fastest.
Arguments:
- lane_source_signal: bfloat16 [1024, 1024], P('tp', 'sp'), may hold values from -6 to 6
- spectral_damping_part: float32 [64, 64], P('tp'), may hold values from -3 to -0.0002
- spectral_angular_part: float32 [64, 64], P('tp'), may hold values from 0.31 to 201.0624
- interval_exponent: float32 [64], P('tp'), may hold values from -3.9 to -1.6
- entry_matrix_inphase: float32 [64, 64, 16], P('tp'), may hold values from -1 to 1
- entry_matrix_quadrature: float32 [64, 64, 16], P('tp'), may hold values from -1 to 1
- emission_inphase: float32 [64, 16, 64], P('tp'), may hold values from -0.75 to 0.75
- emission_quadrature: float32 [64, 16, 64], P('tp'), may hold values from -0.75 to 0.75
- lane_bypass_factor: float32 [1024], P('tp'), may hold values from -5 to 5
- spike_shrink_offset: float32 [64, 1024], P('tp', 'sp'), may hold values from -1.4 to 0
- lane_exit_matrix: bfloat16 [1024, 4096], P('tp'), may hold values from -0.1875 to 0.1875
- skipline_stream: bfloat16 [1024, 4096], P('sp'), may hold values from -6 to 6
- specialist_scaling_vector: float32 [4096], replicated, may hold values from 0.1 to 1.9
- selected_specialists: int32 [1024, 2], P('sp'), may hold values from 0 to 7, all different within a row; in each aligned block of 128 rows (0 to 127, 128 to 255, ...) at most 64 rows name the same one
- dispatcher_scores: float32 [1024, 2], P('sp'), may hold values from 0.1 to 1
- specialist_valve_matrix: bfloat16 [8, 4096, 2048], P('sp', None, 'tp'), may hold values from -0.09375 to 0.09375
- specialist_widen_matrix: bfloat16 [8, 4096, 2048], P('sp', None, 'tp'), may hold values from -0.09375 to 0.09375
- specialist_shrink_matrix: bfloat16 [8, 2048, 4096], P('sp', 'tp'), may hold values from -0.1875 to 0.1875
Outputs:
- updated: bfloat16 [1024, 4096], P('sp', 'tp')
The draws below stay inside these ranges and needn't reach their ends.
Inputs may be any that keep to these rules, and one draw needn't show every extreme that they name: `selected_specialists`: each row names 2 different experts. Among the rows of each aligned block of 128 positions no expert is named more than 64 times, and in every block some expert is named exactly 64 times.
All inputs are finite; a program needn't handle non-finite values.
Results may differ from the reference program's by a relative error of at most 0.019.
Values may be sent and summed in bfloat16 or wider, within the bound.
A program may use at most 64 MiB of HBM per device.

```python
import math
import jax
import jax.numpy as jnp
import numpy as np
from jax import lax

D = 4096
C = 1024
GS = 16
P_SIZE = 64
F = 2048
TOPK = 2
TOK_DEV = 128
G = 64
TOKENS = 1024
EXPERTS = 8
CAP = 64
N_SP = 8
N_TP = 4


def draw_spectral_damping_part(key, part):
    subkeys = jax.random.split(key, 3)
    fast_group = jax.random.uniform(subkeys[0], (G, 1)) < 0.5
    quick_rate = -jax.random.uniform(subkeys[1], (G, P_SIZE), jnp.float32, 1.0, 3.0)
    slow_rate = -jnp.exp(jax.random.uniform(subkeys[2], (G, P_SIZE), jnp.float32, math.log(0.0002), math.log(0.001)))
    return jnp.where(fast_group, quick_rate, slow_rate)


def draw_spectral_angular_part(key, part):
    offset = jax.random.uniform(key, (G, P_SIZE), jnp.float32, 0.1, 0.9)
    return math.pi * (jnp.arange(P_SIZE, dtype=jnp.float32)[None, :] + offset)


def draw_spike_shrink_offset(key, part):
    subkeys = jax.random.split(key, 3)
    blocks = TOKENS // 32
    block_rate = jnp.exp(jax.random.uniform(subkeys[0], (G, blocks), jnp.float32, math.log(2.5e-05), math.log(0.0001)))
    baseline = -jnp.repeat(block_rate, 32, axis=1)
    spots = jax.random.randint(subkeys[1], (G, 2), 0, TOKENS)
    losses = jnp.log(1.0 - jax.random.uniform(subkeys[2], (G, 2), jnp.float32, 0.2, 0.5))
    position = jnp.arange(TOKENS, dtype=jnp.int32)[None, :, None]
    struck = position == spots[:, None, :]
    return baseline + jnp.sum(jnp.where(struck, losses[:, None, :], 0.0), axis=2)


def raised(result, stream_key, source, target, shards_of, factor):
    owner, partner = [(jnp.arange(result.shape[dim]) // (result.shape[dim] // shards_of)).reshape([-1 if axis == dim else 1 for axis in range(result.ndim)]) for dim in (source, target)]
    chosen = jax.random.permutation(stream_key, shards_of)[partner]
    strong = (owner == chosen) | (owner == (partner + shards_of // 2) % shards_of)
    return jnp.where(strong, factor * result, result)


def steps_of(stream_key, shape, cuts, smallest, top_value):
    def one(dim, shards_of):
        steps = jax.random.uniform(jax.random.fold_in(jax.random.fold_in(stream_key, 6), dim), (shards_of,), jnp.float32, smallest / len(cuts), top_value / len(cuts))
        return jnp.repeat(jnp.exp(steps), shape[dim] // shards_of).reshape((-1,) + (1,) * (len(shape) - dim - 1))

    factor_of = one(*cuts[0])
    for cut in cuts[1:]:
        factor_of = factor_of * one(*cut)
    return factor_of


def assign_block(rng, own, number, rows, number_of, top, most, skew):
    sequence = jax.random.permutation(rng, number_of)
    crowded, common = shares(number_of, rows * top, most, skew, True), shares(number_of, rows * top, most, skew, False)
    places = jnp.arange(number_of)

    def named(tallies, turn):
        used = int((tallies > 0).sum())
        fixed = max(1, used // 4)
        moved = fixed + (places - fixed + turn * (used - fixed)) % max(1, number_of - fixed)
        return jnp.zeros((number_of,), jnp.int32).at[sequence[jnp.where(places < fixed, places, moved)]].set(jnp.asarray(tallies, jnp.int32))

    tallies = jnp.where(number % 4 == 0, named(crowded, number // 4), named(common, number - number // 4 - 1))
    mixed = jax.random.permutation(jax.random.fold_in(own, 3), number_of)
    giver, sink = mixed[0:number_of // 2 * 2:2], mixed[1:number_of // 2 * 2:2]
    slack = jnp.minimum(tallies[giver] - 1, most - tallies[sink]) // 2
    slack = jnp.where((giver == sequence[0]) | (sink == sequence[0]) | (tallies[sink] == 0), 0, jnp.maximum(slack, 0))
    moved = jax.random.randint(jax.random.fold_in(own, 4), (number_of // 2,), 0, 1 << 20) % (slack + 1)
    tallies = tallies.at[giver].add(-moved).at[sink].add(moved)
    members = jnp.searchsorted(jnp.cumsum(tallies), jnp.arange(rows * top), side="right").astype(jnp.int32)
    listing = members.reshape(top, rows).T
    listing = listing[jax.random.permutation(jax.random.fold_in(own, 1), rows)]
    turn = jax.random.randint(jax.random.fold_in(own, 2), (rows, 1), 0, top)
    return jnp.take_along_axis(listing, (jnp.arange(top)[None, :] + turn) % top, axis=1)


def shares(number_of, total, reach, lean, full):
    loads = [(1 << 20) // math.isqrt(grade ** lean) + 1 for grade in range(1, number_of + 1)]
    largest = reach if full else min(reach, max(-(-total // number_of), total * loads[0] // sum(loads)))
    least = 1 if total - largest >= number_of - 1 else 0
    given, surplus = [largest] + [least] * (number_of - 1), total - largest - least * (number_of - 1)
    while surplus > 0:
        free = [i for i in range(1, number_of) if given[i] < largest] or [i for i in range(1, number_of) if given[i] < reach]
        whole, left = sum([loads[i] for i in free]), surplus
        for i in free:
            more = min(reach - given[i], max(1, left * loads[i] // whole), surplus)
            given[i] = given[i] + more
            surplus = surplus - more
    return np.array(given)


def centred(key, shape, width, most, pieces=(), kind=jnp.bfloat16):
    gain = steps_of(key, shape, pieces, -0.22, 0.18) if pieces else 1.0
    result = jax.random.normal(key, shape, jnp.float32) * width * gain
    return jnp.minimum(jnp.maximum(result, -most), most).astype(kind)


def heavy_noise(own_key, extent, width, most, shards, heavy, kind=jnp.bfloat16):
    array = width * jax.random.normal(own_key, extent, jnp.float32)
    if shards:
        array = array * steps_of(own_key, extent, shards, -0.22, 0.18)
    return jnp.clip(raised(array, jax.random.fold_in(own_key, 3), *heavy), -most, most).astype(kind)


def setup_inputs(seed: int = 0) -> dict:
    streams_of = jax.random.split(jax.random.key(seed), 19)
    lane_source_signal = centred(streams_of[0], (C, TOKENS), 1.0, 6.0, ((0, 4), (1, 8)))
    spectral_damping_part = draw_spectral_damping_part(jax.random.fold_in(streams_of[18], 71), 0)
    spectral_angular_part = draw_spectral_angular_part(jax.random.fold_in(streams_of[18], 71), 0)
    interval_exponent = jnp.clip(-3.9 + 2.3000001 * jax.random.uniform(streams_of[3], (G,), jnp.float32) ** steps_of(streams_of[3], (G,), ((0, 4),), -0.2, 0.2), -3.9, -1.6)
    entry_matrix_inphase = centred(streams_of[4], (G, P_SIZE, GS), (2 * GS) ** -0.5, 1.0, ((0, 4),), jnp.float32)
    entry_matrix_quadrature = centred(streams_of[5], (G, P_SIZE, GS), (2 * GS) ** -0.5, 1.0, ((0, 4),), jnp.float32)
    emission_inphase = centred(streams_of[6], (G, GS, P_SIZE), P_SIZE ** -0.5, 0.75, ((0, 4),), jnp.float32)
    emission_quadrature = centred(streams_of[7], (G, GS, P_SIZE), P_SIZE ** -0.5, 0.75, ((0, 4),), jnp.float32)
    lane_bypass_factor = centred(streams_of[8], (C,), 1.0, 5.0, ((0, 4),), jnp.float32)
    spike_shrink_offset = draw_spike_shrink_offset(jax.random.fold_in(streams_of[18], 71), 0)
    lane_exit_matrix = centred(streams_of[10], (C, D), C ** -0.5, 0.1875, ((0, 4),))
    skipline_stream = centred(streams_of[11], (TOKENS, D), 1.0, 6.0, ((0, 8),))
    specialist_scaling_vector = jnp.clip(1.0 + 0.18 * jax.random.normal(streams_of[12], (D,), jnp.float32), 0.1, 1.9)
    selected_specialists_keys = jax.random.split(jax.random.fold_in(streams_of[13], 1), TOKENS // TOK_DEV)
    selected_specialists_turns = jax.random.permutation(jax.random.fold_in(streams_of[13], 3), TOKENS // TOK_DEV)
    selected_specialists = jax.vmap(lambda own, number: assign_block(jax.random.fold_in(streams_of[13], 2), own, number, TOK_DEV, EXPERTS, TOPK, CAP, 2))(selected_specialists_keys, selected_specialists_turns).reshape((TOKENS, TOPK))
    dispatcher_scores = jnp.clip(jnp.exp(math.log(1.0) - 2.3025851 * jax.random.uniform(streams_of[14], (TOKENS, TOPK), jnp.float32) ** steps_of(streams_of[14], (TOKENS, TOPK), ((0, 8),), -0.2, 0.2)), 0.1, 1.0)
    specialist_valve_matrix = centred(streams_of[15], (EXPERTS, D, F), D ** -0.5, 0.09375, ((0, 8), (2, 4)))
    specialist_widen_matrix = centred(streams_of[16], (EXPERTS, D, F), D ** -0.5, 0.09375, ((0, 8), (2, 4)))
    specialist_shrink_matrix = heavy_noise(streams_of[17], (EXPERTS, F, D), F ** -0.5, 0.1875, ((0, 8), (1, 4)), (1, 2, 4, 2.0))
    return {"lane_source_signal": lane_source_signal, "spectral_damping_part": spectral_damping_part, "spectral_angular_part": spectral_angular_part, "interval_exponent": interval_exponent, "entry_matrix_inphase": entry_matrix_inphase, "entry_matrix_quadrature": entry_matrix_quadrature, "emission_inphase": emission_inphase, "emission_quadrature": emission_quadrature, "lane_bypass_factor": lane_bypass_factor, "spike_shrink_offset": spike_shrink_offset, "lane_exit_matrix": lane_exit_matrix, "skipline_stream": skipline_stream, "specialist_scaling_vector": specialist_scaling_vector, "selected_specialists": selected_specialists, "dispatcher_scores": dispatcher_scores, "specialist_valve_matrix": specialist_valve_matrix, "specialist_widen_matrix": specialist_widen_matrix, "specialist_shrink_matrix": specialist_shrink_matrix}


EPS = 1e-06
PRECISE_MODE = lax.Precision.HIGHEST

def affine_pair(earlier, latter):
    mul_re = earlier[0] * latter[0] - earlier[1] * latter[1]
    mul_im = earlier[0] * latter[1] + earlier[1] * latter[0]
    add_re = latter[0] * earlier[2] - latter[1] * earlier[3] + latter[2]
    add_im = latter[0] * earlier[3] + latter[1] * earlier[2] + latter[3]
    return (mul_re, mul_im, add_re, add_im)

def bundled_recurrence_layer(packed):
    u_group, a_real, a_imag, log_dt, b_real, b_imag, c_real, c_imag, skip_group, extra_row = packed
    step_size = jnp.exp(log_dt)
    natural_pace_exponent = a_real * step_size
    angle = a_imag * step_size
    num_re = jnp.expm1(natural_pace_exponent) * jnp.cos(angle) - 2.0 * jnp.sin(0.5 * angle) ** 2
    num_im = jnp.exp(natural_pace_exponent) * jnp.sin(angle)
    denom = a_real * a_real + a_imag * a_imag
    fac_re = (num_re * a_real + num_im * a_imag) / denom
    fac_im = (num_im * a_real - num_re * a_imag) / denom
    map_re = fac_re[:, None] * b_real - fac_im[:, None] * b_imag
    map_im = fac_re[:, None] * b_imag + fac_im[:, None] * b_real
    drive_re = jnp.dot(map_re, u_group, precision=PRECISE_MODE)
    drive_im = jnp.dot(map_im, u_group, precision=PRECISE_MODE)
    recurrence_modulus = jnp.exp(natural_pace_exponent[:, None] + extra_row[None, :])
    trans_re = recurrence_modulus * jnp.cos(angle)[:, None]
    trans_im = recurrence_modulus * jnp.sin(angle)[:, None]
    scanned = lax.associative_scan(affine_pair, (trans_re, trans_im, drive_re, drive_im), axis=1)
    value = jnp.dot(c_real, scanned[2], precision=PRECISE_MODE) - jnp.dot(c_imag, scanned[3], precision=PRECISE_MODE) + skip_group[:, None] * u_group
    return jax.nn.gelu(value).astype(jnp.bfloat16)

def reference(lane_source_signal, spectral_damping_part, spectral_angular_part, interval_exponent, entry_matrix_inphase, entry_matrix_quadrature, emission_inphase, emission_quadrature, lane_bypass_factor, spike_shrink_offset, lane_exit_matrix, skipline_stream, specialist_scaling_vector, selected_specialists, dispatcher_scores, specialist_valve_matrix, specialist_widen_matrix, specialist_shrink_matrix):
    f32 = jnp.float32
    bf16 = jnp.bfloat16
    bundle_total = spectral_damping_part.shape[0]
    lanes_within_bundle = entry_matrix_inphase.shape[2]
    length = lane_source_signal.shape[1]
    bundled_signal = lane_source_signal.astype(f32).reshape(bundle_total, lanes_within_bundle, length)
    recurrence_result = lax.map(bundled_recurrence_layer, (bundled_signal, spectral_damping_part, spectral_angular_part, interval_exponent, entry_matrix_inphase, entry_matrix_quadrature, emission_inphase, emission_quadrature, lane_bypass_factor.reshape(bundle_total, lanes_within_bundle), spike_shrink_offset))
    recurrence_result = recurrence_result.reshape(bundle_total * lanes_within_bundle, length)
    projected = jnp.dot(recurrence_result.T, lane_exit_matrix, preferred_element_type=f32).astype(bf16)
    stream = (skipline_stream.astype(f32) + lax.optimization_barrier(projected).astype(f32)).astype(bf16)
    stream_f = lax.optimization_barrier(stream).astype(f32)
    inv_rms = lax.rsqrt(lax.optimization_barrier(jnp.mean(stream_f * stream_f, axis=-1, keepdims=True)) + EPS)
    normed = (stream_f * inv_rms * specialist_scaling_vector).astype(bf16)
    share = dispatcher_scores / lax.optimization_barrier(jnp.sum(dispatcher_scores, axis=1, keepdims=True))
    flat_routes = selected_specialists.reshape(-1)
    flat_share = share.reshape(-1)
    slots = N_SP * CAP
    block_units = F // N_TP

    def one_expert(total, packed):
        gate_w, up_w, down_w, expert_id = packed
        chosen = flat_routes == expert_id
        positions = jnp.nonzero(chosen, size=slots, fill_value=0)[0].astype(jnp.int32)
        valid = jnp.arange(slots, dtype=jnp.int32) < jnp.sum(chosen.astype(jnp.int32))
        token_ids = positions // TOPK
        rows = normed[token_ids]
        gate_part = jnp.dot(rows, gate_w, preferred_element_type=f32)
        up_part = jnp.dot(rows, up_w, preferred_element_type=f32)
        hidden = (jax.nn.silu(gate_part) * up_part).astype(bf16)
        hidden_blocks = jnp.transpose(hidden.reshape(slots, N_TP, block_units), (1, 0, 2))
        down_blocks = down_w.reshape(N_TP, block_units, down_w.shape[1])

        def add_block(acc, pair):
            part = jnp.dot(pair[0], pair[1], preferred_element_type=f32).astype(bf16)
            return (acc + lax.optimization_barrier(part).astype(f32), None)
        acc0 = jnp.zeros((slots, down_w.shape[1]), f32)
        summed, _ = lax.scan(add_block, acc0, (hidden_blocks, down_blocks))
        expert_out = lax.optimization_barrier(summed.astype(bf16)).astype(f32)
        weights = jnp.where(valid, flat_share[positions], 0.0)
        return (total.at[token_ids].add(weights[:, None] * expert_out), None)
    start = jnp.zeros(stream_f.shape, f32)
    experts = specialist_valve_matrix.shape[0]
    moe, _ = lax.scan(one_expert, start, (specialist_valve_matrix, specialist_widen_matrix, specialist_shrink_matrix, jnp.arange(experts, dtype=jnp.int32)))
    return (stream_f + moe).astype(bf16)
```

```python
import jax
import jax.numpy as jnp
from jax import lax
from jax.experimental import pallas as pl
from jax.experimental.pallas import tpu as pltpu
from jax.sharding import PartitionSpec as P

EPS = 1e-06
PRECISE_MODE = lax.Precision.HIGHEST


MESH = pl.DeviceIdType.MESH
VM = pl.BlockSpec(memory_space=pltpu.VMEM)
DMA = pltpu.SemaphoreType.DMA
VMEM_ROOM = 60 * 1024 * 1024


def greet(peers):
    barrier = pltpu.get_barrier_semaphore()
    for peer in peers:
        pl.semaphore_signal(barrier, inc=1, device_id=peer, device_id_type=MESH)
    pl.semaphore_wait(barrier, len(peers))


def remote(src, dst, send, recv, where):
    return pltpu.make_async_remote_copy(
        src_ref=src, dst_ref=dst, send_sem=send, recv_sem=recv, device_id=where, device_id_type=MESH
    )


def places():
    n_sp, n_tp = lax.axis_size("sp"), lax.axis_size("tp")
    return n_sp, n_tp, lax.axis_index("sp"), lax.axis_index("tp")


def carry_kernel(mine, out, pieces, send, recv):
    n_sp, n_tp, me, lane = places()
    greet([(lax.rem(me + i, n_sp), lane) for i in range(1, n_sp)])
    copies = []
    for i in range(1, n_sp):
        copy = remote(
            mine, pieces.at[i - 1], send.at[i - 1], recv.at[i - 1], (lax.rem(me + i, n_sp), lane)
        )
        copy.start()
        copies.append(copy)
    for copy in copies:
        copy.wait_recv()
    run_re = jnp.zeros(mine.shape[1:], jnp.float32)
    run_im = run_re
    for i in range(n_sp - 1, 0, -1):
        mul_re, mul_im, add_re, add_im = (pieces[i - 1, plane] for plane in range(4))
        new_re = mul_re * run_re - mul_im * run_im + add_re
        new_im = mul_re * run_im + mul_im * run_re + add_im
        run_re = jnp.where(me >= i, new_re, run_re)
        run_im = jnp.where(me >= i, new_im, run_im)
    out[0] = run_re
    out[1] = run_im
    for copy in copies:
        copy.wait_send()


def carry_call(summary):
    n_sp = lax.axis_size("sp")
    return pl.pallas_call(
        carry_kernel,
        out_shape=jax.ShapeDtypeStruct((2,) + summary.shape[1:], jnp.float32),
        in_specs=[VM],
        out_specs=VM,
        scratch_shapes=[
            pltpu.VMEM((n_sp - 1,) + summary.shape, jnp.float32),
            DMA((n_sp - 1,)),
            DMA((n_sp - 1,)),
        ],
        compiler_params=pltpu.CompilerParams(collective_id=0, has_side_effects=True),
        name="carry",
    )(summary)


def tp_peers(n_tp, me, lane):
    return [(me, lax.rem(lane + i, n_tp)) for i in range(1, n_tp)]


def sp_peers(n_sp, me, lane):
    return [(lax.rem(me + i, n_sp), lane) for i in range(1, n_sp)]


def dispatch_kernel(
    rows, w, skip, gain, hot,
    stream_out, xs,
    psend, precv, ysend, yrecv, ssend, srecv, dsend,
    ps, pr, ys, yr, ss, sr, ds, dr, fs, fr, qs, qr,
):
    f32, bf16 = jnp.float32, jnp.bfloat16
    n_sp, n_tp, me, lane = places()
    n_y = n_tp // 2
    y, core = lane // 2, lax.rem(lane, 2)
    partner = (me, y * 2 + 1 - core)
    d_local = stream_out.shape[1]
    cap = hot.shape[0] // n_sp
    greet(tp_peers(n_tp, me, lane) + sp_peers(n_sp, me, lane))

    def cols(block):
        return pl.ds(pl.multiple_of(block * d_local, 128), d_local)

    def rows_of(source):
        return pl.ds(pl.multiple_of(source * cap, 16), cap)

    def part(block):
        return jnp.dot(rows[...], w[:, cols(block)], preferred_element_type=f32)

    def y_at(i):
        return lax.rem(y + i, n_y)

    waits = []

    def go(copy):
        copy.start()
        waits.append(copy)
        return copy

    pair = []
    for i in range(n_y - 1, -1, -1):
        psend[i] = part(y_at(i) * 2 + 1 - core).astype(bf16)
        pair.append(go(remote(psend.at[i], precv.at[i], ps.at[i], pr.at[i], partner)))
    pair = pair[::-1]
    across = []
    for i in range(n_y - 1, 0, -1):
        own = part(y_at(i) * 2 + core)
        pair[i].wait_recv()
        ysend[i - 1] = (own + precv[i].astype(f32)).astype(bf16)
        across.append(
            go(
                remote(
                    ysend.at[i - 1], yrecv.at[i - 1], ys.at[i - 1], yr.at[i - 1],
                    (me, y_at(i) * 2 + core),
                )
            )
        )
    total = part(lane)
    pair[0].wait_recv()
    total = total + precv[0].astype(f32)
    for i, copy in enumerate(across[::-1]):
        copy.wait_recv()
        total = total + yrecv[i].astype(f32)
    projected = total.astype(bf16).astype(f32)
    stream = (skip[:, cols(lane)].astype(f32) + projected).astype(bf16)
    stream_out[...] = stream
    stream_f = stream.astype(f32)
    tok = stream_f.shape[0]
    square = jnp.sum(stream_f * stream_f, axis=1, keepdims=True)
    as_rows = jnp.broadcast_to(square, (tok, 128)).T[0:8, :]
    ssend[...] = as_rows
    sums = []
    for i in range(1, n_tp):
        sums.append(
            go(
                remote(
                    ssend, srecv.at[i - 1], ss.at[i - 1], sr.at[i - 1], (me, lax.rem(lane + i, n_tp))
                )
            )
        )
    for i, copy in enumerate(sums):
        copy.wait_recv()
        as_rows = as_rows + srecv[i]
    width = n_tp * d_local
    inv = lax.rsqrt(as_rows / width + EPS)
    inv_rms = jnp.broadcast_to(inv[0:1, :], (128, tok)).T[:, 0:1]
    normed = (stream_f * inv_rms * gain[0:1, cols(lane)]).astype(bf16)

    out_cols = cols(lane)
    arrivals = []
    for i in range(1, n_sp):
        to = lax.rem(me + i, n_sp)
        dsend[i - 1] = jnp.dot(hot[rows_of(to), :], normed, preferred_element_type=f32).astype(bf16)
        arrivals.append(
            go(
                remote(
                    dsend.at[i - 1], xs.at[rows_of(me), out_cols], ds.at[i - 1], dr.at[i - 1],
                    (to, lane),
                )
            )
        )
    xs[rows_of(me), out_cols] = jnp.dot(
        hot[rows_of(me), :], normed, preferred_element_type=f32
    ).astype(bf16)

    def spread(n, source):
        there = xs.at[rows_of(source), out_cols]
        for i in range(1, n_y):
            k = (i - 1) * n_sp + n
            go(remote(there, there, fs.at[k], fr.at[k], (me, y_at(i) * 2 + core)))
        go(remote(there, there, qs.at[n], qr.at[n], partner))

    def source_at(n):
        return lax.rem(me + n_sp - n, n_sp)

    def landed(source, block, recv, send):
        here = xs.at[rows_of(source), cols(block)]
        remote(here, here, send, recv, partner).wait_recv()

    spread(0, me)
    for n in range(1, n_sp):
        landed(source_at(n), lane, dr.at[n - 1], ds.at[n - 1])
        spread(n, source_at(n))
    for n in range(n_sp):
        for i in range(1, n_y):
            k = (i - 1) * n_sp + n
            from_block = lax.rem(y + n_y - i, n_y) * 2 + core
            landed(source_at(n), from_block, fr.at[k], fs.at[k])
            here = xs.at[rows_of(source_at(n)), cols(from_block)]
            q = i * n_sp + n
            go(remote(here, here, qs.at[q], qr.at[q], partner))
    for n in range(n_sp):
        for i in range(n_y):
            from_block = lax.rem(y + n_y - i, n_y) * 2 + 1 - core
            q = i * n_sp + n
            landed(source_at(n), from_block, qr.at[q], qs.at[q])
    for copy in waits:
        copy.wait_send()


def dispatch_call(rows, w, skip, gain, hot):
    n_sp, n_tp = lax.axis_size("sp"), lax.axis_size("tp")
    n_y = n_tp // 2
    bf16, f32 = jnp.bfloat16, jnp.float32
    tok, width = skip.shape
    d_local = width // n_tp
    slots = hot.shape[0]
    cap = slots // n_sp
    more = max(n_y - 1, 1)
    return pl.pallas_call(
        dispatch_kernel,
        out_shape=(
            jax.ShapeDtypeStruct((tok, d_local), bf16),
            jax.ShapeDtypeStruct((slots, width), bf16),
        ),
        in_specs=[VM] * 5,
        out_specs=(VM, VM),
        scratch_shapes=[
            pltpu.VMEM((n_y, tok, d_local), bf16),
            pltpu.VMEM((n_y, tok, d_local), bf16),
            pltpu.VMEM((more, tok, d_local), bf16),
            pltpu.VMEM((more, tok, d_local), bf16),
            pltpu.VMEM((8, tok), f32),
            pltpu.VMEM((n_tp - 1, 8, tok), f32),
            pltpu.VMEM((n_sp - 1, cap, d_local), bf16),
            DMA((n_y,)),
            DMA((n_y,)),
            DMA((more,)),
            DMA((more,)),
            DMA((n_tp - 1,)),
            DMA((n_tp - 1,)),
            DMA((n_sp - 1,)),
            DMA((n_sp - 1,)),
            DMA((more * n_sp,)),
            DMA((more * n_sp,)),
            DMA((n_y * n_sp,)),
            DMA((n_y * n_sp,)),
        ],
        compiler_params=pltpu.CompilerParams(
            collective_id=1, has_side_effects=True, vmem_limit_bytes=VMEM_ROOM
        ),
        name="dispatch",
    )(rows, w, skip, gain, hot)


def return_kernel(
    down, stream, share, pick,
    out,
    precv, ysend, yrecv, rsend, ret,
    ps, pr, ys, yr, rs, rr,
):
    f32, bf16 = jnp.float32, jnp.bfloat16
    n_sp, n_tp, me, lane = places()
    n_y = n_tp // 2
    y, core = lane // 2, lax.rem(lane, 2)
    partner = (me, y * 2 + 1 - core)
    d_local = out.shape[1]
    cap = down.shape[0] // n_sp
    greet(
        [partner]
        + [(me, lax.rem(y + i, n_y) * 2 + core) for i in range(1, n_y)]
        + sp_peers(n_sp, me, lane)
    )

    def cols(block):
        return pl.ds(pl.multiple_of(block * d_local, 128), d_local)

    def rows_of(source):
        return pl.ds(pl.multiple_of(source * cap, 16), cap)

    def y_at(i):
        return lax.rem(y + i, n_y)

    def to_at(n):
        return lax.rem(me + n + 1, n_sp)

    waits = []

    def go(copy):
        copy.start()
        waits.append(copy)
        return copy

    pair, across, back = {}, {}, []
    for n in range(n_sp):
        for i in list(range(1, n_y)) + [0]:
            k = n * n_y + i
            src = down.at[rows_of(to_at(n)), cols(y_at(i) * 2 + 1 - core)]
            pair[n, i] = go(remote(src, precv.at[k], ps.at[k], pr.at[k], partner))
    for n in range(n_sp):
        for i in range(1, n_y):
            pair[n, i].wait_recv()
            k = n * (n_y - 1) + i - 1
            mine = down[rows_of(to_at(n)), cols(y_at(i) * 2 + core)].astype(f32)
            ysend[k] = (mine + precv[n * n_y + i].astype(f32)).astype(bf16)
            across[n, i] = go(
                remote(
                    ysend.at[k], yrecv.at[k], ys.at[k], yr.at[k], (me, y_at(i) * 2 + core)
                )
            )
    for n in range(n_sp):
        total = down[rows_of(to_at(n)), cols(lane)].astype(f32)
        pair[n, 0].wait_recv()
        total = total + precv[n * n_y].astype(f32)
        for i in range(1, n_y):
            across[n, i].wait_recv()
            total = total + yrecv[n * (n_y - 1) + i - 1].astype(f32)
        if n < n_sp - 1:
            rsend[n] = total.astype(bf16)
            back.append(
                go(remote(rsend.at[n], ret.at[rows_of(me), :], rs.at[n], rr.at[n], (to_at(n), lane)))
            )
        else:
            ret[rows_of(me), :] = total.astype(bf16)
    for n in range(n_sp - 1):
        here = ret.at[rows_of(lax.rem(me + n_sp - n - 1, n_sp)), :]
        remote(here, here, rs.at[n], rr.at[n], partner).wait_recv()
    combined = stream[...].astype(f32)
    rows_in = ret[...]
    moe = None
    for k in range(pick.shape[0]):
        chosen = jnp.dot(pick[k], rows_in, preferred_element_type=f32) * share[:, k : k + 1]
        moe = chosen if moe is None else moe + chosen
    out[...] = (combined + moe).astype(bf16)
    for copy in waits:
        copy.wait_send()


def return_call(down, stream, share, pick):
    n_sp, n_tp = lax.axis_size("sp"), lax.axis_size("tp")
    n_y = n_tp // 2
    bf16 = jnp.bfloat16
    tok, d_local = stream.shape
    slots = down.shape[0]
    cap = slots // n_sp
    more = max((n_y - 1) * n_sp, 1)
    return pl.pallas_call(
        return_kernel,
        out_shape=jax.ShapeDtypeStruct((tok, d_local), bf16),
        in_specs=[VM] * 4,
        out_specs=VM,
        scratch_shapes=[
            pltpu.VMEM((n_y * n_sp, cap, d_local), bf16),
            pltpu.VMEM((more, cap, d_local), bf16),
            pltpu.VMEM((more, cap, d_local), bf16),
            pltpu.VMEM((n_sp - 1, cap, d_local), bf16),
            pltpu.VMEM((slots, d_local), bf16),
            DMA((n_y * n_sp,)),
            DMA((n_y * n_sp,)),
            DMA((more,)),
            DMA((more,)),
            DMA((n_sp - 1,)),
            DMA((n_sp - 1,)),
        ],
        compiler_params=pltpu.CompilerParams(
            collective_id=2, has_side_effects=True, vmem_limit_bytes=VMEM_ROOM
        ),
        name="combine",
    )(down, stream, share, pick)


def affine_pair(earlier, latter):
    mul_re = earlier[0] * latter[0] - earlier[1] * latter[1]
    mul_im = earlier[0] * latter[1] + earlier[1] * latter[0]
    add_re = latter[0] * earlier[2] - latter[1] * earlier[3] + latter[2]
    add_im = latter[0] * earlier[3] + latter[1] * earlier[2] + latter[3]
    return (mul_re, mul_im, add_re, add_im)


def local_prefix(elements):
    length = elements[0].shape[2]
    fills = (1.0, 0.0, 0.0, 0.0)
    offset = 1
    while offset < length:
        earlier = tuple(
            (
                jnp.pad(
                    item[:, :, : length - offset],
                    ((0, 0), (0, 0), (offset, 0)),
                    constant_values=fill,
                )
                for item, fill in zip(elements, fills)
            )
        )
        elements = affine_pair(earlier, elements)
        offset = offset * 2
    return elements


def per_device(
    lane_source_signal,
    spectral_damping_part,
    spectral_angular_part,
    interval_exponent,
    entry_matrix_inphase,
    entry_matrix_quadrature,
    emission_inphase,
    emission_quadrature,
    lane_bypass_factor,
    spike_shrink_offset,
    lane_exit_matrix,
    skipline_stream,
    specialist_scaling_vector,
    selected_specialists,
    dispatcher_scores,
    specialist_valve_matrix,
    specialist_widen_matrix,
    specialist_shrink_matrix,
):
    f32 = jnp.float32
    bf16 = jnp.bfloat16
    groups_here = spectral_damping_part.shape[0]
    lanes_within_bundle = entry_matrix_inphase.shape[2]
    tok_local = lane_source_signal.shape[1]
    bundled_signal = lane_source_signal.astype(f32).reshape(
        groups_here, lanes_within_bundle, tok_local
    )
    step_size = jnp.exp(interval_exponent)[:, None]
    natural_pace_exponent = spectral_damping_part * step_size
    angle = spectral_angular_part * step_size
    num_re = jnp.expm1(natural_pace_exponent) * jnp.cos(angle) - 2.0 * jnp.sin(0.5 * angle) ** 2
    num_im = jnp.exp(natural_pace_exponent) * jnp.sin(angle)
    denom = (
        spectral_damping_part * spectral_damping_part
        + spectral_angular_part * spectral_angular_part
    )
    fac_re = (num_re * spectral_damping_part + num_im * spectral_angular_part) / denom
    fac_im = (num_im * spectral_damping_part - num_re * spectral_angular_part) / denom
    map_re = (
        fac_re[:, :, None] * entry_matrix_inphase - fac_im[:, :, None] * entry_matrix_quadrature
    )
    map_im = (
        fac_re[:, :, None] * entry_matrix_quadrature + fac_im[:, :, None] * entry_matrix_inphase
    )
    drive_re = jnp.einsum("gpc,gct->gpt", map_re, bundled_signal, precision=PRECISE_MODE)
    drive_im = jnp.einsum("gpc,gct->gpt", map_im, bundled_signal, precision=PRECISE_MODE)
    recurrence_modulus = jnp.exp(
        natural_pace_exponent[:, :, None] + spike_shrink_offset[:, None, :]
    )
    trans_re = recurrence_modulus * jnp.cos(angle)[:, :, None]
    trans_im = recurrence_modulus * jnp.sin(angle)[:, :, None]
    cum_re, cum_im, state_real, state_imaginary = local_prefix(
        (trans_re, trans_im, drive_re, drive_im)
    )
    summary = jnp.stack(
        [
            plane[:, :, -1].reshape(-1, 128)
            for plane in (cum_re, cum_im, state_real, state_imaginary)
        ]
    )
    entering = carry_call(summary)
    enter_re = entering[0].reshape(groups_here, -1)[:, :, None]
    enter_im = entering[1].reshape(groups_here, -1)[:, :, None]
    state_real = state_real + cum_re * enter_re - cum_im * enter_im
    state_imaginary = state_imaginary + cum_re * enter_im + cum_im * enter_re
    value = (
        jnp.einsum("nef,nfi->nei", emission_inphase, state_real, precision=PRECISE_MODE)
        - jnp.einsum("nef,nfi->nei", emission_quadrature, state_imaginary, precision=PRECISE_MODE)
        + lane_bypass_factor.reshape(groups_here, lanes_within_bundle)[:, :, None] * bundled_signal
    )
    recurrence_result = (
        jax.nn.gelu(value).astype(bf16).reshape(groups_here * lanes_within_bundle, tok_local)
    )
    share = dispatcher_scores / jnp.sum(dispatcher_scores, axis=1, keepdims=True)
    experts = lax.axis_size("sp")
    top = selected_specialists.shape[1]
    capacity = 2 * tok_local * top // experts
    flat_routes = selected_specialists.reshape(-1)
    hits = (flat_routes[:, None] == jnp.arange(experts, dtype=jnp.int32)[None, :]).astype(jnp.int32)
    ranks = jnp.sum((jnp.cumsum(hits, axis=0) - hits) * hits, axis=1)
    slot_ids = (flat_routes * capacity + ranks).reshape(tok_local, top)
    slot_grid = jnp.arange(experts * capacity, dtype=jnp.int32)
    pick = jnp.stack(
        [(slot_ids[:, k : k + 1] == slot_grid[None, :]).astype(bf16) for k in range(top)]
    )
    hot = jnp.any(slot_grid[:, None, None] == slot_ids.T[None, :, :], axis=1).astype(bf16)
    stream, rows = dispatch_call(
        recurrence_result.T,
        lane_exit_matrix,
        skipline_stream,
        specialist_scaling_vector[None, :],
        hot,
    )
    gate_part = jnp.dot(rows, specialist_valve_matrix[0], preferred_element_type=f32)
    up_part = jnp.dot(rows, specialist_widen_matrix[0], preferred_element_type=f32)
    hidden = (jax.nn.silu(gate_part) * up_part).astype(bf16)
    down_part = jnp.dot(hidden, specialist_shrink_matrix[0], preferred_element_type=f32).astype(bf16)
    return return_call(down_part, stream, share, pick)


def solution(mesh):
    placed = (
        P("tp", "sp"),
        P("tp", None),
        P("tp", None),
        P("tp"),
        P("tp", None, None),
        P("tp", None, None),
        P("tp", None, None),
        P("tp", None, None),
        P("tp"),
        P("tp", "sp"),
        P("tp", None),
        P("sp", None),
        P(),
        P("sp", None),
        P("sp", None),
        P("sp", None, "tp"),
        P("sp", None, "tp"),
        P("sp", "tp", None),
    )
    return jax.shard_map(
        per_device, mesh=mesh, in_specs=placed, out_specs=P("sp", "tp"), check_vma=False
    )
```

```python
import jax
import jax.numpy as jnp
from jax import lax
from jax.experimental import pallas as pl
from jax.experimental.pallas import tpu as pltpu
from jax.sharding import PartitionSpec as P

EPS = 1e-06
PRECISE_MODE = lax.Precision.HIGHEST


MESH = pl.DeviceIdType.MESH
VM = pl.BlockSpec(memory_space=pltpu.VMEM)
DMA = pltpu.SemaphoreType.DMA
VMEM_ROOM = 48 * 1024 * 1024


def greet(peers):
    barrier = pltpu.get_barrier_semaphore()
    for peer in peers:
        pl.semaphore_signal(barrier, inc=1, device_id=peer, device_id_type=MESH)
    pl.semaphore_wait(barrier, len(peers))


def remote(src, dst, send, recv, where):
    return pltpu.make_async_remote_copy(
        src_ref=src, dst_ref=dst, send_sem=send, recv_sem=recv, device_id=where, device_id_type=MESH
    )


def places():
    n_sp, n_tp = lax.axis_size("sp"), lax.axis_size("tp")
    return n_sp, n_tp, lax.axis_index("sp"), lax.axis_index("tp")


def carry_kernel(mine, out, pieces, send, recv):
    n_sp, n_tp, me, lane = places()
    greet([(lax.rem(me + i, n_sp), lane) for i in range(1, n_sp)])
    copies = []
    for i in range(1, n_sp):
        copy = remote(
            mine, pieces.at[i - 1], send.at[i - 1], recv.at[i - 1], (lax.rem(me + i, n_sp), lane)
        )
        copy.start()
        copies.append(copy)
    for copy in copies:
        copy.wait_recv()
    run_re = jnp.zeros(mine.shape[1:], jnp.float32)
    run_im = run_re
    for i in range(n_sp - 1, 0, -1):
        mul_re, mul_im, add_re, add_im = (pieces[i - 1, plane] for plane in range(4))
        new_re = mul_re * run_re - mul_im * run_im + add_re
        new_im = mul_re * run_im + mul_im * run_re + add_im
        run_re = jnp.where(me >= i, new_re, run_re)
        run_im = jnp.where(me >= i, new_im, run_im)
    out[0] = run_re
    out[1] = run_im
    for copy in copies:
        copy.wait_send()


def carry_call(summary):
    n_sp = lax.axis_size("sp")
    return pl.pallas_call(
        carry_kernel,
        out_shape=jax.ShapeDtypeStruct((2,) + summary.shape[1:], jnp.float32),
        in_specs=[VM],
        out_specs=VM,
        scratch_shapes=[
            pltpu.VMEM((n_sp - 1,) + summary.shape, jnp.float32),
            DMA((n_sp - 1,)),
            DMA((n_sp - 1,)),
        ],
        compiler_params=pltpu.CompilerParams(collective_id=0, has_side_effects=True),
        name="carry",
    )(summary)


def tp_peers(n_tp, me, lane):
    return [(me, lax.rem(lane + i, n_tp)) for i in range(1, n_tp)]


def sp_peers(n_sp, me, lane):
    return [(lax.rem(me + i, n_sp), lane) for i in range(1, n_sp)]


def dispatch_kernel(
    rows, w, skip, gain, hot,
    stream_out, xs,
    psend, precv, ysend, yrecv, ssend, srecv, dsend,
    ps, pr, ys, yr, ss, sr, ds, dr, fs, fr, qs, qr,
):
    f32, bf16 = jnp.float32, jnp.bfloat16
    n_sp, n_tp, me, lane = places()
    n_y = n_tp // 2
    y, core = lane // 2, lax.rem(lane, 2)
    partner = (me, y * 2 + 1 - core)
    d_local = stream_out.shape[1]
    cap = hot.shape[0] // n_sp
    greet(tp_peers(n_tp, me, lane) + sp_peers(n_sp, me, lane))

    def cols(block):
        return pl.ds(pl.multiple_of(block * d_local, 128), d_local)

    def rows_of(source):
        return pl.ds(pl.multiple_of(source * cap, 16), cap)

    def part(block):
        return jnp.dot(rows[...], w[:, cols(block)], preferred_element_type=f32)

    def y_at(i):
        return lax.rem(y + i, n_y)

    waits = []

    def go(copy):
        copy.start()
        waits.append(copy)
        return copy

    pair = []
    for i in range(n_y - 1, -1, -1):
        psend[i] = part(y_at(i) * 2 + 1 - core).astype(bf16)
        pair.append(go(remote(psend.at[i], precv.at[i], ps.at[i], pr.at[i], partner)))
    pair = pair[::-1]
    across = []
    for i in range(n_y - 1, 0, -1):
        own = part(y_at(i) * 2 + core)
        pair[i].wait_recv()
        ysend[i - 1] = (own + precv[i].astype(f32)).astype(bf16)
        across.append(
            go(
                remote(
                    ysend.at[i - 1], yrecv.at[i - 1], ys.at[i - 1], yr.at[i - 1],
                    (me, y_at(i) * 2 + core),
                )
            )
        )
    total = part(lane)
    pair[0].wait_recv()
    total = total + precv[0].astype(f32)
    for i, copy in enumerate(across[::-1]):
        copy.wait_recv()
        total = total + yrecv[i].astype(f32)
    projected = total.astype(bf16).astype(f32)
    stream = (skip[:, cols(lane)].astype(f32) + projected).astype(bf16)
    stream_out[...] = stream
    stream_f = stream.astype(f32)
    tok = stream_f.shape[0]
    square = jnp.sum(stream_f * stream_f, axis=1, keepdims=True)
    as_rows = jnp.broadcast_to(square, (tok, 128)).T[0:8, :]
    ssend[...] = as_rows
    sums = []
    for i in range(1, n_tp):
        sums.append(
            go(
                remote(
                    ssend, srecv.at[i - 1], ss.at[i - 1], sr.at[i - 1], (me, lax.rem(lane + i, n_tp))
                )
            )
        )
    for i, copy in enumerate(sums):
        copy.wait_recv()
        as_rows = as_rows + srecv[i]
    width = n_tp * d_local
    inv = lax.rsqrt(as_rows / width + EPS)
    inv_rms = jnp.broadcast_to(inv[0:1, :], (128, tok)).T[:, 0:1]
    normed = (stream_f * inv_rms * gain[0:1, cols(lane)]).astype(bf16)

    out_cols = cols(lane)
    arrivals = []
    for i in range(1, n_sp):
        to = lax.rem(me + i, n_sp)
        dsend[i - 1] = jnp.dot(hot[rows_of(to), :], normed, preferred_element_type=f32).astype(bf16)
        arrivals.append(
            go(
                remote(
                    dsend.at[i - 1], xs.at[rows_of(me), out_cols], ds.at[i - 1], dr.at[i - 1],
                    (to, lane),
                )
            )
        )
    xs[rows_of(me), out_cols] = jnp.dot(
        hot[rows_of(me), :], normed, preferred_element_type=f32
    ).astype(bf16)

    def spread(n, source):
        there = xs.at[rows_of(source), out_cols]
        for i in range(1, n_y):
            k = (i - 1) * n_sp + n
            go(remote(there, there, fs.at[k], fr.at[k], (me, y_at(i) * 2 + core)))
        go(remote(there, there, qs.at[n], qr.at[n], partner))

    def source_at(n):
        return lax.rem(me + n_sp - n, n_sp)

    def landed(source, block, recv, send):
        here = xs.at[rows_of(source), cols(block)]
        remote(here, here, send, recv, partner).wait_recv()

    spread(0, me)
    for n in range(1, n_sp):
        landed(source_at(n), lane, dr.at[n - 1], ds.at[n - 1])
        spread(n, source_at(n))
    for n in range(n_sp):
        for i in range(1, n_y):
            k = (i - 1) * n_sp + n
            from_block = lax.rem(y + n_y - i, n_y) * 2 + core
            landed(source_at(n), from_block, fr.at[k], fs.at[k])
            here = xs.at[rows_of(source_at(n)), cols(from_block)]
            q = i * n_sp + n
            go(remote(here, here, qs.at[q], qr.at[q], partner))
    for n in range(n_sp):
        for i in range(n_y):
            from_block = lax.rem(y + n_y - i, n_y) * 2 + 1 - core
            q = i * n_sp + n
            landed(source_at(n), from_block, qr.at[q], qs.at[q])
    for copy in waits:
        copy.wait_send()


def dispatch_call(rows, w, skip, gain, hot):
    n_sp, n_tp = lax.axis_size("sp"), lax.axis_size("tp")
    n_y = n_tp // 2
    bf16, f32 = jnp.bfloat16, jnp.float32
    tok, width = skip.shape
    d_local = width // n_tp
    slots = hot.shape[0]
    cap = slots // n_sp
    more = max(n_y - 1, 1)
    return pl.pallas_call(
        dispatch_kernel,
        out_shape=(
            jax.ShapeDtypeStruct((tok, d_local), bf16),
            jax.ShapeDtypeStruct((slots, width), bf16),
        ),
        in_specs=[VM] * 5,
        out_specs=(VM, VM),
        scratch_shapes=[
            pltpu.VMEM((n_y, tok, d_local), bf16),
            pltpu.VMEM((n_y, tok, d_local), bf16),
            pltpu.VMEM((more, tok, d_local), bf16),
            pltpu.VMEM((more, tok, d_local), bf16),
            pltpu.VMEM((8, tok), f32),
            pltpu.VMEM((n_tp - 1, 8, tok), f32),
            pltpu.VMEM((n_sp - 1, cap, d_local), bf16),
            DMA((n_y,)),
            DMA((n_y,)),
            DMA((more,)),
            DMA((more,)),
            DMA((n_tp - 1,)),
            DMA((n_tp - 1,)),
            DMA((n_sp - 1,)),
            DMA((n_sp - 1,)),
            DMA((more * n_sp,)),
            DMA((more * n_sp,)),
            DMA((n_y * n_sp,)),
            DMA((n_y * n_sp,)),
        ],
        compiler_params=pltpu.CompilerParams(
            collective_id=1, has_side_effects=True, vmem_limit_bytes=VMEM_ROOM // 2
        ),
        name="dispatch",
    )(rows, w, skip, gain, hot)


def return_kernel(
    hidden, w, share, pick,
    out,
    psend, own, precv, ysend, yrecv, rsend, ret,
    ps, pr, ys, yr, rs, rr,
):
    f32, bf16 = jnp.float32, jnp.bfloat16
    n_sp, n_tp, me, lane = places()
    n_y = n_tp // 2
    y, core = lane // 2, lax.rem(lane, 2)
    partner = (me, y * 2 + 1 - core)
    d_local = out.shape[1]
    cap = hidden.shape[0] // n_sp
    greet(
        [partner]
        + [(me, lax.rem(y + i, n_y) * 2 + core) for i in range(1, n_y)]
        + sp_peers(n_sp, me, lane)
    )

    def cols(block):
        return pl.ds(pl.multiple_of(block * d_local, 128), d_local)

    def rows_of(source):
        return pl.ds(pl.multiple_of(source * cap, 16), cap)

    def y_at(i):
        return lax.rem(y + i, n_y)

    def to_at(n):
        return lax.rem(me + n + 1, n_sp)

    waits = []

    def go(copy):
        copy.start()
        waits.append(copy)
        return copy

    pair, across, back = {}, {}, []
    def part(n, block):
        return jnp.dot(hidden[rows_of(to_at(n)), :], w[:, cols(block)], preferred_element_type=f32)

    order = list(range(1, n_y)) + [0]
    for n in range(n_sp + 1):
        if n < n_sp:
            for i in order:
                k = n * n_y + i
                psend[k] = part(n, y_at(i) * 2 + 1 - core).astype(bf16)
                pair[n, i] = go(remote(psend.at[k], precv.at[k], ps.at[k], pr.at[k], partner))
            for i in order:
                own[n * n_y + i] = part(n, y_at(i) * 2 + core)
        if n > 0:
            for i in range(1, n_y):
                pair[n - 1, i].wait_recv()
                j = (n - 1) * n_y + i
                k = (n - 1) * (n_y - 1) + i - 1
                ysend[k] = (own[j] + precv[j].astype(f32)).astype(bf16)
                across[n - 1, i] = go(
                    remote(
                        ysend.at[k], yrecv.at[k], ys.at[k], yr.at[k], (me, y_at(i) * 2 + core)
                    )
                )
    for n in range(n_sp):
        total = own[n * n_y]
        pair[n, 0].wait_recv()
        total = total + precv[n * n_y].astype(f32)
        for i in range(1, n_y):
            across[n, i].wait_recv()
            total = total + yrecv[n * (n_y - 1) + i - 1].astype(f32)
        if n < n_sp - 1:
            rsend[n] = total.astype(bf16)
            back.append(
                go(remote(rsend.at[n], ret.at[rows_of(me), :], rs.at[n], rr.at[n], (to_at(n), lane)))
            )
        else:
            ret[rows_of(me), :] = total.astype(bf16)
    for n in range(n_sp - 1):
        here = ret.at[rows_of(lax.rem(me + n_sp - n - 1, n_sp)), :]
        remote(here, here, rs.at[n], rr.at[n], partner).wait_recv()
    rows_in = ret[...]
    moe = None
    for k in range(pick.shape[0]):
        chosen = jnp.dot(pick[k], rows_in, preferred_element_type=f32) * share[:, k : k + 1]
        moe = chosen if moe is None else moe + chosen
    out[...] = moe
    for copy in waits:
        copy.wait_send()


def return_call(hidden, w, share, pick):
    n_sp, n_tp = lax.axis_size("sp"), lax.axis_size("tp")
    n_y = n_tp // 2
    bf16, f32 = jnp.bfloat16, jnp.float32
    tok, d_local = share.shape[0], w.shape[1] // n_tp
    slots = hidden.shape[0]
    cap = slots // n_sp
    more = max((n_y - 1) * n_sp, 1)
    return pl.pallas_call(
        return_kernel,
        out_shape=jax.ShapeDtypeStruct((tok, d_local), f32),
        in_specs=[VM] * 4,
        out_specs=VM,
        scratch_shapes=[
            pltpu.VMEM((n_y * n_sp, cap, d_local), bf16),
            pltpu.VMEM((n_y * n_sp, cap, d_local), f32),
            pltpu.VMEM((n_y * n_sp, cap, d_local), bf16),
            pltpu.VMEM((more, cap, d_local), bf16),
            pltpu.VMEM((more, cap, d_local), bf16),
            pltpu.VMEM((n_sp - 1, cap, d_local), bf16),
            pltpu.VMEM((slots, d_local), bf16),
            DMA((n_y * n_sp,)),
            DMA((n_y * n_sp,)),
            DMA((more,)),
            DMA((more,)),
            DMA((n_sp - 1,)),
            DMA((n_sp - 1,)),
        ],
        compiler_params=pltpu.CompilerParams(
            collective_id=2, has_side_effects=True, vmem_limit_bytes=VMEM_ROOM
        ),
        name="combine",
    )(hidden, w, share, pick)


def affine_pair(earlier, latter):
    mul_re = earlier[0] * latter[0] - earlier[1] * latter[1]
    mul_im = earlier[0] * latter[1] + earlier[1] * latter[0]
    add_re = latter[0] * earlier[2] - latter[1] * earlier[3] + latter[2]
    add_im = latter[0] * earlier[3] + latter[1] * earlier[2] + latter[3]
    return (mul_re, mul_im, add_re, add_im)


def local_prefix(elements):
    length = elements[0].shape[2]
    fills = (1.0, 0.0, 0.0, 0.0)
    offset = 1
    while offset < length:
        earlier = tuple(
            (
                jnp.pad(
                    item[:, :, : length - offset],
                    ((0, 0), (0, 0), (offset, 0)),
                    constant_values=fill,
                )
                for item, fill in zip(elements, fills)
            )
        )
        elements = affine_pair(earlier, elements)
        offset = offset * 2
    return elements


def per_device(
    lane_source_signal,
    spectral_damping_part,
    spectral_angular_part,
    interval_exponent,
    entry_matrix_inphase,
    entry_matrix_quadrature,
    emission_inphase,
    emission_quadrature,
    lane_bypass_factor,
    spike_shrink_offset,
    lane_exit_matrix,
    skipline_stream,
    specialist_scaling_vector,
    selected_specialists,
    dispatcher_scores,
    specialist_valve_matrix,
    specialist_widen_matrix,
    specialist_shrink_matrix,
):
    f32 = jnp.float32
    bf16 = jnp.bfloat16
    groups_here = spectral_damping_part.shape[0]
    lanes_within_bundle = entry_matrix_inphase.shape[2]
    tok_local = lane_source_signal.shape[1]
    bundled_signal = lane_source_signal.astype(f32).reshape(
        groups_here, lanes_within_bundle, tok_local
    )
    step_size = jnp.exp(interval_exponent)[:, None]
    natural_pace_exponent = spectral_damping_part * step_size
    angle = spectral_angular_part * step_size
    num_re = jnp.expm1(natural_pace_exponent) * jnp.cos(angle) - 2.0 * jnp.sin(0.5 * angle) ** 2
    num_im = jnp.exp(natural_pace_exponent) * jnp.sin(angle)
    denom = (
        spectral_damping_part * spectral_damping_part
        + spectral_angular_part * spectral_angular_part
    )
    fac_re = (num_re * spectral_damping_part + num_im * spectral_angular_part) / denom
    fac_im = (num_im * spectral_damping_part - num_re * spectral_angular_part) / denom
    map_re = (
        fac_re[:, :, None] * entry_matrix_inphase - fac_im[:, :, None] * entry_matrix_quadrature
    )
    map_im = (
        fac_re[:, :, None] * entry_matrix_quadrature + fac_im[:, :, None] * entry_matrix_inphase
    )
    drive_re = jnp.einsum("gpc,gct->gpt", map_re, bundled_signal, precision=PRECISE_MODE)
    drive_im = jnp.einsum("gpc,gct->gpt", map_im, bundled_signal, precision=PRECISE_MODE)
    recurrence_modulus = jnp.exp(
        natural_pace_exponent[:, :, None] + spike_shrink_offset[:, None, :]
    )
    trans_re = recurrence_modulus * jnp.cos(angle)[:, :, None]
    trans_im = recurrence_modulus * jnp.sin(angle)[:, :, None]
    cum_re, cum_im, state_real, state_imaginary = local_prefix(
        (trans_re, trans_im, drive_re, drive_im)
    )
    summary = jnp.stack(
        [
            plane[:, :, -1].reshape(-1, 128)
            for plane in (cum_re, cum_im, state_real, state_imaginary)
        ]
    )
    entering = carry_call(summary)
    enter_re = entering[0].reshape(groups_here, -1)[:, :, None]
    enter_im = entering[1].reshape(groups_here, -1)[:, :, None]
    state_real = state_real + cum_re * enter_re - cum_im * enter_im
    state_imaginary = state_imaginary + cum_re * enter_im + cum_im * enter_re
    value = (
        jnp.einsum("nef,nfi->nei", emission_inphase, state_real, precision=PRECISE_MODE)
        - jnp.einsum("nef,nfi->nei", emission_quadrature, state_imaginary, precision=PRECISE_MODE)
        + lane_bypass_factor.reshape(groups_here, lanes_within_bundle)[:, :, None] * bundled_signal
    )
    recurrence_result = (
        jax.nn.gelu(value).astype(bf16).reshape(groups_here * lanes_within_bundle, tok_local)
    )
    share = dispatcher_scores / jnp.sum(dispatcher_scores, axis=1, keepdims=True)
    experts = lax.axis_size("sp")
    top = selected_specialists.shape[1]
    capacity = 2 * tok_local * top // experts
    flat_routes = selected_specialists.reshape(-1)
    hits = (flat_routes[:, None] == jnp.arange(experts, dtype=jnp.int32)[None, :]).astype(jnp.int32)
    ranks = jnp.sum((jnp.cumsum(hits, axis=0) - hits) * hits, axis=1)
    slot_ids = (flat_routes * capacity + ranks).reshape(tok_local, top)
    slot_grid = jnp.arange(experts * capacity, dtype=jnp.int32)
    pick = jnp.stack(
        [(slot_ids[:, k : k + 1] == slot_grid[None, :]).astype(bf16) for k in range(top)]
    )
    hot = jnp.any(slot_grid[:, None, None] == slot_ids.T[None, :, :], axis=1).astype(bf16)
    stream, rows = dispatch_call(
        recurrence_result.T,
        lane_exit_matrix,
        skipline_stream,
        specialist_scaling_vector[None, :],
        hot,
    )
    gate_part = jnp.dot(rows, specialist_valve_matrix[0], preferred_element_type=f32)
    up_part = jnp.dot(rows, specialist_widen_matrix[0], preferred_element_type=f32)
    hidden = (jax.nn.silu(gate_part) * up_part).astype(bf16)
    moe = return_call(hidden, specialist_shrink_matrix[0], share, pick)
    return (stream.astype(f32) + moe).astype(bf16)


def solution(mesh):
    placed = (
        P("tp", "sp"),
        P("tp", None),
        P("tp", None),
        P("tp"),
        P("tp", None, None),
        P("tp", None, None),
        P("tp", None, None),
        P("tp", None, None),
        P("tp"),
        P("tp", "sp"),
        P("tp", None),
        P("sp", None),
        P(),
        P("sp", None),
        P("sp", None),
        P("sp", None, "tp"),
        P("sp", None, "tp"),
        P("sp", "tp", None),
    )
    return jax.shard_map(
        per_device, mesh=mesh, in_specs=placed, out_specs=P("sp", "tp"), check_vma=False
    )
```
